32 devices in a mesh: sp: 16 (over z, y, x), tp: 2 (over core).
Axes of the slice: x: 2, y: 2, z: 4, core: 2. Of those that a mesh axis runs over, the one named last changes fastest.
Arguments:
- queries: bfloat16 [4096, 1024], P('sp', 'tp'), may hold values from -100 to 100
- keys: bfloat16 [256, 4096], P('tp', 'sp'), may hold values from -5 to 5
- values: bfloat16 [256, 4096], P('tp', 'sp'), may hold values from -4.5 to 4.5
- gate_cache: float32 [8, 4096], P('tp', 'sp'), as said below
- documents: int32 [4096], P('sp'), may hold values from 0 to 2, never falling along the last dimension, each value on 1 to 2560 neighbouring positions
- residual: bfloat16 [4096, 2048], P(('sp', 'tp')), may hold values from -3 to 3
- out_weight: bfloat16 [1024, 2048], replicated, may hold values from -2 to 2
- mix_gain: bfloat16 [2048], replicated, may hold values from 0.099609375 to 1.8984375
- routes: int32 [4096, 4], P(('sp', 'tp')), may hold values from 0 to 31, all different within a row; in each aligned block of 128 rows (0 to 127, 128 to 255, ...) at most 32 rows name the same one
- route_weight: float32 [4096, 4], P(('sp', 'tp')), may hold values from 0.25 to 1
- expert_gate: bfloat16 [32, 2048, 512], P(('sp', 'tp')), may hold values from -0.125 to 0.125
- expert_up: bfloat16 [32, 2048, 512], P(('sp', 'tp')), may hold values from -0.125 to 0.125
- expert_down: bfloat16 [32, 512, 2048], P(('sp', 'tp')), may hold values from -0.25 to 0.25
- shared_gate: bfloat16 [2048, 512], replicated, may hold values from -0.125 to 0.125
- shared_up: bfloat16 [2048, 512], replicated, may hold values from -0.125 to 0.125
- shared_down: bfloat16 [512, 2048], replicated, may hold values from -0.25 to 0.25
- ffn_gain: bfloat16 [2048], replicated, may hold values from 0.099609375 to 1.8984375
Outputs:
- result: bfloat16 [4096, 2048], P(('sp', 'tp'))
The draws below stay inside these ranges and needn't reach their ends.
Inputs may be any that keep to these rules, and one draw needn't show every extreme that they name: `gate_cache`: entry (h, j) is the sum of head h's log forget gates over positions 0 to j. `documents`: never falls along the positions; no document has more than 2560 positions. `routes`: each row names 4 different experts; in the rows of one device (aligned blocks of 128 rows) no expert is named more than 32 times, a bound that some block reaches.
All inputs are finite; a program needn't handle non-finite values.
Results may differ from the reference program's by a relative error of at most 0.013.
Values may be sent and summed in bfloat16 or wider, within the bound.
A program may use at most 256 MiB of HBM per device.

```python
import math
import jax
import jax.numpy as jnp
import numpy as np
from jax import lax

D = 2048
HEADS = 8
KV_HEADS = 2
HD = 128
EFF = 512
SFF = 512
TOPK = 4
DOCS = 3
TOK_DEV = 256
SEQUENCE_TOKENS = 4096
ROWS = 128
EXPERTS = 32
CAP = 32
DOC_MOST = 2560


def attention_draw(key):
    sequence_pieces = jax.random.split(jax.random.fold_in(key, 7), 2)
    key_rows = jnp.clip(jax.random.normal(sequence_pieces[0], (KV_HEADS, HD, SEQUENCE_TOKENS), jnp.float32), -4.5, 4.5)
    query_rows = jnp.clip(jax.random.normal(sequence_pieces[1], (SEQUENCE_TOKENS, HEADS, HD), jnp.float32), -4.5, 4.5)
    return (query_rows.reshape(SEQUENCE_TOKENS, HEADS * HD), key_rows.reshape(KV_HEADS * HD, SEQUENCE_TOKENS))


def draw_queries(key, part):
    return attention_draw(key)[0].astype(jnp.bfloat16)


def draw_keys(key, part):
    return attention_draw(key)[1].astype(jnp.bfloat16)


def draw_gate_cache(key, part):
    sequence_pieces = jax.random.split(jax.random.fold_in(key, 11), 7)
    ordering = jax.random.permutation(sequence_pieces[0], HEADS)
    fast_count = HEADS // 2
    is_fast = ordering < fast_count
    blocks = SEQUENCE_TOKENS // TOK_DEV
    block_rate = jnp.exp(jax.random.uniform(sequence_pieces[1], (HEADS, blocks), jnp.float32, -0.7, 0.7))
    block_rate = jnp.repeat(block_rate, TOK_DEV, axis=1)
    roughness = jax.random.uniform(sequence_pieces[2], (HEADS, SEQUENCE_TOKENS), jnp.float32, 0.2, 1.8)
    slow_rate = jax.random.uniform(sequence_pieces[3], (HEADS, 1), jnp.float32, 0.3, 0.7) / SEQUENCE_TOKENS
    fast_rate = 1.0 / jax.random.uniform(sequence_pieces[4], (HEADS, 1), jnp.float32, 30.0, 100.0)
    decay_rates = jnp.where(is_fast[:, None], fast_rate, slow_rate) * block_rate * roughness
    surge_position = jax.random.randint(sequence_pieces[5], (3,), 0, SEQUENCE_TOKENS)
    token_surges = jnp.any(jnp.arange(SEQUENCE_TOKENS)[None, :] == surge_position[:, None], axis=0)
    loss_values = -jnp.log(1.0 - jax.random.uniform(sequence_pieces[6], (HEADS, 1), jnp.float32, 0.2, 0.35))
    gate_logarithms = -decay_rates - jnp.where(token_surges[None, :], loss_values, 0.0)
    return jnp.cumsum(gate_logarithms, axis=1)


def steps_of(stream_key, extent, pieces, low, high):
    factor_of, own = 1.0, jax.random.fold_in(stream_key, 6)
    for position, shards_of in pieces:
        steps = jnp.exp(jax.random.uniform(jax.random.fold_in(own, position), (shards_of,), jnp.float32, low / len(pieces), high / len(pieces)))
        factor_of = factor_of * jnp.repeat(steps, extent[position] // shards_of).reshape([-1 if axis == position else 1 for axis in range(len(extent))])
    return factor_of


def length_profile(count, total, bound, slope):
    loads = [(1 << 20) // math.isqrt(grade ** slope) + 1 for grade in range(2, count + 1)]
    spare, holding = total - bound - (count - 1), [1] * (count - 1)
    while spare > 0:
        movable = [i for i in range(count - 1) if holding[i] < bound]
        whole, left = sum([loads[i] for i in movable]), spare
        for i in movable:
            addition = min(bound - holding[i], max(1, left * loads[i] // whole), spare)
            holding[i] = holding[i] + addition
            spare = spare - addition
    return np.array([bound] + holding)


def uneven_parts(key, amount, total, bound, lean):
    if amount == 2:
        one = jax.random.randint(key, (), max(1, total - bound), min(bound, total - 1) + 1)
        return jnp.stack([one, total - one])
    sizes = jnp.asarray(length_profile(amount, total, bound, lean), jnp.int32)
    twos = (amount - 1) // 2
    giver, taker = sizes[1:1 + 2 * twos:2], sizes[2:2 + 2 * twos:2]
    slack = jnp.minimum(giver - 1, bound - taker)
    passed = jax.random.randint(jax.random.fold_in(key, 1), (twos,), 0, 1 << 20) % (slack + 1)
    sizes = sizes.at[1:1 + 2 * twos:2].set(giver - passed).at[2:2 + 2 * twos:2].set(taker + passed)
    return sizes[jax.random.permutation(jax.random.fold_in(key, 2), amount)]


def assign_block(rng, own, number, rows, number_of, top, most, lean):
    sequence = jax.random.permutation(rng, number_of)
    heavy_load, usual = portions_of(number_of, rows * top, most, lean, True), portions_of(number_of, rows * top, most, lean, False)
    places = jnp.arange(number_of)

    def named(sizes, offset_by):
        used = int((sizes > 0).sum())
        fixed = max(1, used // 4)
        passed = fixed + (places - fixed + offset_by * (used - fixed)) % max(1, number_of - fixed)
        return jnp.zeros((number_of,), jnp.int32).at[sequence[jnp.where(places < fixed, places, passed)]].set(jnp.asarray(sizes, jnp.int32))

    sizes = jnp.where(number % 4 == 0, named(heavy_load, number // 4), named(usual, number - number // 4 - 1))
    mixed = jax.random.permutation(jax.random.fold_in(own, 3), number_of)
    giver, sink = mixed[0:number_of // 2 * 2:2], mixed[1:number_of // 2 * 2:2]
    slack = jnp.minimum(sizes[giver] - 1, most - sizes[sink]) // 2
    slack = jnp.where((giver == sequence[0]) | (sink == sequence[0]) | (sizes[sink] == 0), 0, jnp.maximum(slack, 0))
    passed = jax.random.randint(jax.random.fold_in(own, 4), (number_of // 2,), 0, 1 << 20) % (slack + 1)
    sizes = sizes.at[giver].add(-passed).at[sink].add(passed)
    members = jnp.searchsorted(jnp.cumsum(sizes), jnp.arange(rows * top), side="right").astype(jnp.int32)
    listing = members.reshape(top, rows).T
    listing = listing[jax.random.permutation(jax.random.fold_in(own, 1), rows)]
    offset_by = jax.random.randint(jax.random.fold_in(own, 2), (rows, 1), 0, top)
    return jnp.take_along_axis(listing, (jnp.arange(top)[None, :] + offset_by) % top, axis=1)


def portions_of(count, total, reach, slope, full):
    loads = [(1 << 20) // math.isqrt(rank ** slope) + 1 for rank in range(1, count + 1)]
    largest = reach if full else min(reach, max(-(-total // count), total * loads[0] // sum(loads)))
    least = 1 if total - largest >= count - 1 else 0
    given, spare = [largest] + [least] * (count - 1), total - largest - least * (count - 1)
    while spare > 0:
        candidates = [i for i in range(1, count) if given[i] < largest] or [i for i in range(1, count) if given[i] < reach]
        mass, remaining = sum([loads[i] for i in candidates]), spare
        for i in candidates:
            more = min(reach - given[i], max(1, remaining * loads[i] // mass), spare)
            given[i] = given[i] + more
            spare = spare - more
    return np.array(given)


def gaussian(own_key, extent, deviation, most, cuts=(), held_as=jnp.bfloat16):
    level = steps_of(own_key, extent, cuts, -0.22, 0.18) if cuts else 1.0
    array = jax.random.normal(own_key, extent, jnp.float32) * deviation * level
    return jnp.minimum(jnp.maximum(array, -most), most).astype(held_as)


def setup_inputs(seed: int = 0) -> dict:
    arg_keys = jax.random.split(jax.random.key(seed), 18)
    queries = draw_queries(jax.random.fold_in(arg_keys[17], 71), 0)
    keys = draw_keys(jax.random.fold_in(arg_keys[17], 71), 0)
    values = gaussian(arg_keys[2], (KV_HEADS * HD, SEQUENCE_TOKENS), 1.0, 4.5, ((0, 2), (1, 16)))
    gate_cache = draw_gate_cache(jax.random.fold_in(arg_keys[17], 71), 0)
    documents = jnp.searchsorted(jnp.cumsum(uneven_parts(arg_keys[4], DOCS, SEQUENCE_TOKENS, DOC_MOST, 0)), jnp.arange(SEQUENCE_TOKENS), side="right").astype(jnp.int32)
    residual = gaussian(arg_keys[5], (SEQUENCE_TOKENS, D), 0.5, 3.0, ((0, 32),))
    out_weight = gaussian(arg_keys[6], (HEADS * HD, D), (4.0 / (HEADS * HD) ** 0.5), 2.0)
    mix_gain = jnp.clip(1.0 + 0.18 * jax.random.normal(arg_keys[7], (D,), jnp.float32), 0.099609375, 1.8984375).astype(jnp.bfloat16)
    routes_keys = jax.random.split(jax.random.fold_in(arg_keys[8], 1), SEQUENCE_TOKENS // ROWS)
    routes_turns = jax.random.permutation(jax.random.fold_in(arg_keys[8], 3), SEQUENCE_TOKENS // ROWS)
    routes = jax.vmap(lambda own, number: assign_block(jax.random.fold_in(arg_keys[8], 2), own, number, ROWS, EXPERTS, TOPK, CAP, 1))(routes_keys, routes_turns).reshape((SEQUENCE_TOKENS, TOPK))
    route_weight = jnp.clip(jnp.exp(math.log(1.0) - 1.3862944 * jax.random.uniform(arg_keys[9], (SEQUENCE_TOKENS, TOPK), jnp.float32) ** steps_of(arg_keys[9], (SEQUENCE_TOKENS, TOPK), ((0, 32),), -0.2, 0.2)), 0.25, 1.0)
    expert_gate = gaussian(arg_keys[10], (EXPERTS, D, EFF), D ** -0.5, 0.125, ((0, 32),))
    expert_up = gaussian(arg_keys[11], (EXPERTS, D, EFF), D ** -0.5, 0.125, ((0, 32),))
    expert_down = gaussian(arg_keys[12], (EXPERTS, EFF, D), EFF ** -0.5, 0.25, ((0, 32),))
    shared_gate = gaussian(arg_keys[13], (D, SFF), D ** -0.5, 0.125)
    shared_up = gaussian(arg_keys[14], (D, SFF), D ** -0.5, 0.125)
    shared_down = gaussian(arg_keys[15], (SFF, D), SFF ** -0.5, 0.25)
    ffn_gain = jnp.clip(1.0 + 0.18 * jax.random.normal(arg_keys[16], (D,), jnp.float32), 0.099609375, 1.8984375).astype(jnp.bfloat16)
    return dict(queries=queries, keys=keys, values=values, gate_cache=gate_cache, documents=documents, residual=residual, out_weight=out_weight, mix_gain=mix_gain, routes=routes, route_weight=route_weight, expert_gate=expert_gate, expert_up=expert_up, expert_down=expert_down, shared_gate=shared_gate, shared_up=shared_up, shared_down=shared_down, ffn_gain=ffn_gain)


residual_scale = 2.0 ** 0.25
norm_epsilon = 1e-05

def normalize(summed, gain_vector):
    row_mean = lax.optimization_barrier(jnp.mean(summed, axis=-1, keepdims=True))
    centred = summed - row_mean
    spread = lax.optimization_barrier(jnp.mean(centred * centred, axis=-1, keepdims=True))
    return (centred * lax.rsqrt(spread + norm_epsilon) * gain_vector.astype(jnp.float32)).astype(jnp.bfloat16)

def attend(queries, keys, values, gate_cache, documents):
    group_size = HEADS // KV_HEADS
    query_full = queries.astype(jnp.float32).reshape(SEQUENCE_TOKENS, KV_HEADS, group_size, HD)
    key_full = keys.astype(jnp.float32).reshape(KV_HEADS, HD, SEQUENCE_TOKENS)
    value_full = values.astype(jnp.float32).reshape(KV_HEADS, HD, SEQUENCE_TOKENS)
    cache = gate_cache.reshape(KV_HEADS, group_size, SEQUENCE_TOKENS)
    key_pos = jnp.arange(SEQUENCE_TOKENS, dtype=jnp.int32)
    score_scale = HD ** (-0.5)

    def block(block_index):
        first_row = (block_index * TOK_DEV).astype(jnp.int32)
        query_block = lax.dynamic_slice_in_dim(query_full, first_row, TOK_DEV, 0)
        query_cum = lax.dynamic_slice_in_dim(cache, first_row, TOK_DEV, 2)
        query_docs = lax.dynamic_slice_in_dim(documents, first_row, TOK_DEV, 0)
        scores = jnp.einsum('qagd,adk->qagk', query_block, key_full) * score_scale
        scores = scores + jnp.transpose(query_cum, (2, 0, 1))[..., None] - cache[None]
        query_pos = first_row + jnp.arange(TOK_DEV, dtype=jnp.int32)
        allowed = (key_pos[None, :] <= query_pos[:, None]) & (documents[None, :] == query_docs[:, None])
        allowed = allowed[:, None, None, :]
        highest = lax.optimization_barrier(jnp.max(jnp.where(allowed, scores, -jnp.inf), axis=-1, keepdims=True))
        weights = jnp.where(allowed, jnp.exp(scores - highest), 0.0)
        totals = lax.optimization_barrier(jnp.sum(weights, axis=-1))
        rounded = lax.optimization_barrier(weights.astype(jnp.bfloat16)).astype(jnp.float32)
        summed = jnp.einsum('qagk,adk->qagd', rounded, value_full)
        return (summed / totals[..., None]).astype(jnp.bfloat16).reshape(TOK_DEV, HEADS * HD)
    return lax.map(block, jnp.arange(SEQUENCE_TOKENS // TOK_DEV, dtype=jnp.int32)).reshape(SEQUENCE_TOKENS, HEADS * HD)

def experts_apply(settled, routes, route_weight, expert_gate, expert_up, expert_down):
    blocks = SEQUENCE_TOKENS // ROWS
    per_block = routes.reshape(blocks, ROWS * TOPK)
    matches = (per_block[:, :, None] == jnp.arange(EXPERTS, dtype=jnp.int32)[None, None, :]).astype(jnp.int32)
    ranks = lax.optimization_barrier(jnp.sum(jnp.cumsum(matches, axis=1) * matches, axis=2)) - 1
    block_ids = jnp.arange(blocks, dtype=jnp.int32)[:, None]
    slots = (per_block * blocks + block_ids) * CAP + ranks
    owners = block_ids * ROWS + jnp.arange(ROWS * TOPK, dtype=jnp.int32)[None, :] // TOPK
    table = jnp.zeros((EXPERTS * blocks * CAP,), jnp.int32).at[slots.reshape(-1)].set(owners.reshape(-1))
    table = table.reshape(EXPERTS, blocks * CAP)

    def one_expert(expert_index):
        taken = jnp.take(settled, table[expert_index], axis=0)
        gate_part = jnp.dot(taken, expert_gate[expert_index], preferred_element_type=jnp.float32)
        up_part = jnp.dot(taken, expert_up[expert_index], preferred_element_type=jnp.float32)
        hidden = (jax.nn.silu(gate_part) * up_part).astype(jnp.bfloat16)
        return jnp.dot(hidden, expert_down[expert_index], preferred_element_type=jnp.float32).astype(jnp.bfloat16)
    produced = lax.map(one_expert, jnp.arange(EXPERTS, dtype=jnp.int32)).reshape(EXPERTS * blocks * CAP, D)
    token_slots = slots.reshape(SEQUENCE_TOKENS, TOPK)
    routed = jnp.zeros((SEQUENCE_TOKENS, D), jnp.float32)
    for choice_index in range(TOPK):
        picked = jnp.take(produced, token_slots[:, choice_index], axis=0).astype(jnp.float32)
        routed = routed + picked * route_weight[:, choice_index][:, None]
    return routed

def reference(queries, keys, values, gate_cache, documents, residual, out_weight, mix_gain, routes, route_weight, expert_gate, expert_up, expert_down, shared_gate, shared_up, shared_down, ffn_gain):
    attended = attend(queries, keys, values, gate_cache, documents)
    mixed = jnp.dot(attended, out_weight, preferred_element_type=jnp.float32).astype(jnp.bfloat16)
    mixed = lax.optimization_barrier(mixed).astype(jnp.float32)
    settled = normalize(residual_scale * residual.astype(jnp.float32) + mixed, mix_gain)
    routed = experts_apply(settled, routes, route_weight, expert_gate, expert_up, expert_down)
    shared_gate_part = jnp.dot(settled, shared_gate, preferred_element_type=jnp.float32)
    shared_up_part = jnp.dot(settled, shared_up, preferred_element_type=jnp.float32)
    shared_hidden = (jax.nn.silu(shared_gate_part) * shared_up_part).astype(jnp.bfloat16)
    shared = jnp.dot(shared_hidden, shared_down, preferred_element_type=jnp.float32)
    return normalize(residual_scale * settled.astype(jnp.float32) + routed + shared, ffn_gain)
```

```python
import functools

import jax
import jax.numpy as jnp
from jax import lax
from jax.experimental import pallas as pl
from jax.experimental.pallas import tpu as pltpu
from jax.sharding import PartitionSpec as P

HD = 128


residual_scale = 2.0**0.25
norm_epsilon = 1e-05
masked_score = -1e30


def normalize(summed, gain_vector):
    row_mean = jnp.mean(summed, axis=-1, keepdims=True)
    centred = summed - row_mean
    spread = jnp.mean(centred * centred, axis=-1, keepdims=True)
    return (centred * lax.rsqrt(spread + norm_epsilon) * gain_vector.astype(jnp.float32)).astype(
        jnp.bfloat16
    )


def attend_kernel(
    planes, across, q_ref, kv_ref, aux_ref, gate_ref, doc_ref, out_ref,
    kv_all, aux_all, top, total, acc, own_sem, up_send, up_recv, side_send, side_recv,
):
    heads = gate_ref.shape[1]
    tok_rows = q_ref.shape[0]
    group_size = heads // (kv_ref.shape[0] // (2 * HD))
    kv_rows = kv_ref.shape[0] // 2
    me = lax.axis_index("sp")
    plane = me // across
    column = me % across

    barrier = pltpu.get_barrier_semaphore()

    def greet(other):
        pl.semaphore_signal(
            barrier, inc=1, device_id={"sp": other}, device_id_type=pl.DeviceIdType.MESH
        )

    for offset in range(1, across):
        greet(plane * across + (column + offset) % across)

    @pl.when(plane + 1 < planes)
    def _():
        greet(me + across)

    @pl.when(plane > 0)
    def _():
        greet(me - across)

    peers = across + 1
    pl.semaphore_wait(
        barrier,
        peers - (planes - plane) // planes - (plane + 1) // planes,
    )

    def copies(slot, other, send_sem, recv_sem, index):
        return [
            pltpu.make_async_remote_copy(
                src_ref=ref.at[slot],
                dst_ref=ref.at[slot],
                send_sem=send_sem.at[index, part],
                recv_sem=recv_sem.at[index, part],
                device_id={"sp": other},
                device_id_type=pl.DeviceIdType.MESH,
            )
            for part, ref in enumerate((kv_all, aux_all))
        ]

    own = [
        pltpu.make_async_copy(kv_ref, kv_all.at[me], own_sem.at[0]),
        pltpu.make_async_copy(aux_ref, aux_all.at[me], own_sem.at[1]),
    ]
    for copy in own:
        copy.start()
    top[...] = jnp.full_like(top, masked_score)
    total[...] = jnp.zeros_like(total)
    acc[...] = jnp.zeros_like(acc)
    for copy in own:
        copy.wait()

    def absorb(slot):
        key_pos = slot * tok_rows + lax.broadcasted_iota(jnp.int32, (tok_rows, tok_rows), 1)
        query_pos = me * tok_rows + lax.broadcasted_iota(jnp.int32, (tok_rows, tok_rows), 0)
        allowed = (key_pos <= query_pos) & (aux_all[slot, heads : heads + 1, :] == doc_ref[...])
        for head in range(heads):
            base = head // group_size * HD
            columns = slice(head * HD, (head + 1) * HD)
            key_block = kv_all[slot, base : base + HD, :]
            value_block = kv_all[slot, kv_rows + base : kv_rows + base + HD, :]
            scores = jnp.dot(
                q_ref[:, columns], key_block, preferred_element_type=jnp.float32
            ) * (HD ** (-0.5))
            scores = scores + (gate_ref[:, head : head + 1] - aux_all[slot, head : head + 1, :])
            scores = jnp.where(allowed, scores, masked_score)
            old_top = top[head]
            new_top = jnp.maximum(old_top, jnp.max(scores, axis=1, keepdims=True))
            weights = jnp.where(allowed, jnp.exp(scores - new_top), 0.0)
            shrink = jnp.exp(old_top - new_top)
            top[head] = new_top
            total[head] = total[head] * shrink + jnp.sum(weights, axis=1, keepdims=True)
            acc[:, columns] = acc[:, columns] * shrink + lax.dot_general(
                weights.astype(jnp.bfloat16),
                value_block,
                (((1,), (1,)), ((), ())),
                preferred_element_type=jnp.float32,
            )

    def rise(step, carry):
        @pl.when(plane >= step)
        def _():
            slot = me - step * across

            @pl.when(step > 0)
            def _():
                for copy in copies(slot, me - across, up_send, up_recv, step - 1):
                    copy.wait_recv()

            @pl.when(plane + 1 < planes)
            def _():
                for copy in copies(slot, me + across, up_send, up_recv, step):
                    copy.start()

            for offset in range(1, across):

                @pl.when((step > 0) | (column + offset < across))
                def _():
                    other = plane * across + (column + offset) % across
                    for copy in copies(
                        slot, other, side_send, side_recv, step * across + offset
                    ):
                        copy.start()

            absorb(slot)

        return carry

    lax.fori_loop(0, planes, rise, 0)

    def spread(turn, carry):
        step = turn // (across - 1)
        offset = 1 + turn % (across - 1)

        @pl.when((plane >= step) & ((step > 0) | (column >= offset)))
        def _():
            source = (column + across - offset) % across
            slot = (plane - step) * across + source
            for copy in copies(
                slot, plane * across + source, side_send, side_recv, step * across + offset
            ):
                copy.wait_recv()
            absorb(slot)

        return carry

    lax.fori_loop(0, planes * (across - 1), spread, 0)

    def settle(step, carry):
        @pl.when(plane >= step)
        def _():
            slot = me - step * across

            @pl.when(plane + 1 < planes)
            def _():
                for copy in copies(slot, me + across, up_send, up_recv, step):
                    copy.wait_send()

            for offset in range(1, across):

                @pl.when((step > 0) | (column + offset < across))
                def _():
                    other = plane * across + (column + offset) % across
                    for copy in copies(
                        slot, other, side_send, side_recv, step * across + offset
                    ):
                        copy.wait_send()

        return carry

    lax.fori_loop(0, planes, settle, 0)
    for head in range(heads):
        columns = slice(head * HD, (head + 1) * HD)
        out_ref[:, columns] = (acc[:, columns] / total[head]).astype(out_ref.dtype)


def attend(queries, keys, values, gate_cache, documents):
    tok_rows = queries.shape[0]
    heads = gate_cache.shape[0]
    devices = lax.axis_size("sp")
    planes = min(4, devices)
    across = devices // planes
    aux_rows = (heads + 8) // 8 * 8
    doc_line = documents.astype(jnp.float32)
    packed = jnp.concatenate([keys, values], axis=0)
    aux = jnp.concatenate(
        [
            gate_cache,
            jnp.broadcast_to(doc_line[None, :], (aux_rows - heads, tok_rows)),
        ],
        axis=0,
    )
    vmem = pl.BlockSpec(memory_space=pltpu.VMEM)
    return pl.pallas_call(
        functools.partial(attend_kernel, planes, across),
        out_shape=jax.ShapeDtypeStruct((tok_rows, heads * HD), jnp.bfloat16),
        in_specs=[vmem] * 5,
        out_specs=vmem,
        scratch_shapes=[
            pltpu.VMEM((devices,) + packed.shape, jnp.bfloat16),
            pltpu.VMEM((devices,) + aux.shape, jnp.float32),
            pltpu.VMEM((heads, tok_rows, 1), jnp.float32),
            pltpu.VMEM((heads, tok_rows, 1), jnp.float32),
            pltpu.VMEM((tok_rows, heads * HD), jnp.float32),
            pltpu.SemaphoreType.DMA((2,)),
            pltpu.SemaphoreType.DMA((planes, 2)),
            pltpu.SemaphoreType.DMA((planes, 2)),
            pltpu.SemaphoreType.DMA((planes * across, 2)),
            pltpu.SemaphoreType.DMA((planes * across, 2)),
        ],
        compiler_params=pltpu.CompilerParams(collective_id=0, has_side_effects=True),
        name="attend",
    )(queries, packed, aux, jnp.transpose(gate_cache), doc_line[:, None])


def expert_block(arrived, expert_gate, expert_up, expert_down):
    own_count = expert_gate.shape[0]
    grouped = arrived.reshape(-1, own_count, arrived.shape[1], arrived.shape[2])
    gate_part = jnp.einsum(
        "nemd,edf->nemf", grouped, expert_gate, preferred_element_type=jnp.float32
    )
    up_part = jnp.einsum("nemd,edf->nemf", grouped, expert_up, preferred_element_type=jnp.float32)
    hidden = (jax.nn.silu(gate_part) * up_part).astype(jnp.bfloat16)
    produced = jnp.einsum("nemf,efd->nemd", hidden, expert_down, preferred_element_type=jnp.float32)
    return produced.astype(jnp.bfloat16).reshape(arrived.shape)


def local(
    queries,
    keys,
    values,
    gate_cache,
    documents,
    residual,
    out_weight,
    mix_gain,
    routes,
    route_weight,
    expert_gate,
    expert_up,
    expert_down,
    shared_gate,
    shared_up,
    shared_down,
    ffn_gain,
):
    attended = attend(queries, keys, values, gate_cache, documents)
    token_heads = lax.all_to_all(attended, "tp", split_axis=0, concat_axis=1, tiled=True)
    mixed = jnp.dot(token_heads, out_weight, preferred_element_type=jnp.float32)
    mixed = lax.optimization_barrier(mixed.astype(jnp.bfloat16)).astype(jnp.float32)
    settled = normalize(residual_scale * residual.astype(jnp.float32) + mixed, mix_gain)
    row_count = settled.shape[0]
    width_model = settled.shape[1]
    top_count = routes.shape[1]
    expert_total = lax.axis_size(("sp", "tp")) * expert_gate.shape[0]
    capacity = row_count * lax.axis_size("tp") * top_count // expert_total
    chosen_experts = routes.reshape(-1)
    matches = (
        chosen_experts[:, None] == jnp.arange(expert_total, dtype=jnp.int32)[None, :]
    ).astype(jnp.int32)
    ranks = jnp.sum(jnp.cumsum(matches, axis=0) * matches, axis=1) - 1
    slots = chosen_experts * capacity + ranks
    placing = slots[None, :] == jnp.arange(expert_total * capacity, dtype=jnp.int32)[:, None]
    placing = jnp.any(
        placing.reshape(expert_total * capacity, row_count, top_count), axis=2
    ).astype(jnp.bfloat16)
    outgoing = jnp.dot(placing, settled, preferred_element_type=jnp.float32).astype(jnp.bfloat16)
    outgoing = outgoing.reshape(expert_total, capacity, width_model)
    finished = expert_block(
        lax.all_to_all(outgoing, ("sp", "tp"), split_axis=0, concat_axis=0, tiled=True),
        expert_gate,
        expert_up,
        expert_down,
    )
    returned = lax.all_to_all(finished, ("sp", "tp"), split_axis=0, concat_axis=0, tiled=True)
    returned = returned.reshape(expert_total * capacity, width_model)
    picked_rows = jnp.take(returned, slots, axis=0).reshape(row_count, top_count, width_model)
    routed = jnp.einsum("rkd,rk->rd", picked_rows.astype(jnp.float32), route_weight)
    shared_gate_part = jnp.dot(settled, shared_gate, preferred_element_type=jnp.float32)
    shared_up_part = jnp.dot(settled, shared_up, preferred_element_type=jnp.float32)
    shared_hidden = (jax.nn.silu(shared_gate_part) * shared_up_part).astype(jnp.bfloat16)
    shared = jnp.dot(shared_hidden, shared_down, preferred_element_type=jnp.float32)
    return normalize(residual_scale * settled.astype(jnp.float32) + routed + shared, ffn_gain)


def solution(mesh):
    placed = (
        P("sp", "tp"),
        P("tp", "sp"),
        P("tp", "sp"),
        P("tp", "sp"),
        P("sp"),
        P(("sp", "tp"), None),
        P(),
        P(),
        P(("sp", "tp"), None),
        P(("sp", "tp"), None),
        P(("sp", "tp"), None, None),
        P(("sp", "tp"), None, None),
        P(("sp", "tp"), None, None),
        P(),
        P(),
        P(),
        P(),
    )
    return jax.shard_map(
        local, mesh=mesh, in_specs=placed, out_specs=P(("sp", "tp"), None), check_vma=False
    )
```

```python
import functools

import jax
import jax.numpy as jnp
from jax import lax
from jax.experimental import pallas as pl
from jax.experimental.pallas import tpu as pltpu
from jax.sharding import PartitionSpec as P

HD = 128


residual_scale = 2.0**0.25
norm_epsilon = 1e-05
masked_score = -1e30


def normalize(summed, gain_vector):
    row_mean = jnp.mean(summed, axis=-1, keepdims=True)
    centred = summed - row_mean
    spread = jnp.mean(centred * centred, axis=-1, keepdims=True)
    return (centred * lax.rsqrt(spread + norm_epsilon) * gain_vector.astype(jnp.float32)).astype(
        jnp.bfloat16
    )


def attend_kernel(
    planes, across, q_ref, kv_ref, aux_ref, gate_ref, doc_ref, out_ref,
    kv_all, aux_all, top, total, acc, own_sem, up_send, up_recv, side_send, side_recv,
):
    heads = gate_ref.shape[1]
    tok_rows = q_ref.shape[0]
    group_size = heads // (kv_ref.shape[0] // (2 * HD))
    kv_rows = kv_ref.shape[0] // 2
    me = lax.axis_index("sp")
    plane = me // across
    column = me % across

    barrier = pltpu.get_barrier_semaphore()

    def greet(other):
        pl.semaphore_signal(
            barrier, inc=1, device_id={"sp": other}, device_id_type=pl.DeviceIdType.MESH
        )

    for offset in range(1, across):
        greet(plane * across + (column + offset) % across)

    @pl.when(plane + 1 < planes)
    def _():
        greet(me + across)

    @pl.when(plane > 0)
    def _():
        greet(me - across)

    peers = across + 1
    pl.semaphore_wait(
        barrier,
        peers - (planes - plane) // planes - (plane + 1) // planes,
    )

    def copies(slot, other, send_sem, recv_sem, index):
        return [
            pltpu.make_async_remote_copy(
                src_ref=ref.at[slot],
                dst_ref=ref.at[slot],
                send_sem=send_sem.at[index, part],
                recv_sem=recv_sem.at[index, part],
                device_id={"sp": other},
                device_id_type=pl.DeviceIdType.MESH,
            )
            for part, ref in enumerate((kv_all, aux_all))
        ]

    own = [
        pltpu.make_async_copy(kv_ref, kv_all.at[me], own_sem.at[0]),
        pltpu.make_async_copy(aux_ref, aux_all.at[me], own_sem.at[1]),
    ]
    for copy in own:
        copy.start()
    top[...] = jnp.full_like(top, masked_score)
    total[...] = jnp.zeros_like(total)
    acc[...] = jnp.zeros_like(acc)
    for copy in own:
        copy.wait()

    def absorb(slot):
        key_pos = slot * tok_rows + lax.broadcasted_iota(jnp.int32, (tok_rows, tok_rows), 1)
        query_pos = me * tok_rows + lax.broadcasted_iota(jnp.int32, (tok_rows, tok_rows), 0)
        allowed = (key_pos <= query_pos) & (aux_all[slot, heads : heads + 1, :] == doc_ref[...])
        for head in range(heads):
            base = head // group_size * HD
            columns = slice(head * HD, (head + 1) * HD)
            key_block = kv_all[slot, base : base + HD, :]
            value_block = kv_all[slot, kv_rows + base : kv_rows + base + HD, :]
            scores = jnp.dot(
                q_ref[:, columns], key_block, preferred_element_type=jnp.float32
            ) * (HD ** (-0.5))
            scores = scores + (gate_ref[:, head : head + 1] - aux_all[slot, head : head + 1, :])
            scores = jnp.where(allowed, scores, masked_score)
            old_top = top[head]
            new_top = jnp.maximum(old_top, jnp.max(scores, axis=1, keepdims=True))
            weights = jnp.where(allowed, jnp.exp(scores - new_top), 0.0)
            shrink = jnp.exp(old_top - new_top)
            top[head] = new_top
            total[head] = total[head] * shrink + jnp.sum(weights, axis=1, keepdims=True)
            acc[:, columns] = acc[:, columns] * shrink + lax.dot_general(
                weights.astype(jnp.bfloat16),
                value_block,
                (((1,), (1,)), ((), ())),
                preferred_element_type=jnp.float32,
            )

    def rise(step, carry):
        @pl.when(plane >= step)
        def _():
            slot = me - step * across

            @pl.when(step > 0)
            def _():
                for copy in copies(slot, me - across, up_send, up_recv, step - 1):
                    copy.wait_recv()

            @pl.when(plane + 1 < planes)
            def _():
                for copy in copies(slot, me + across, up_send, up_recv, step):
                    copy.start()

            for offset in range(1, across):

                @pl.when((step > 0) | (column + offset < across))
                def _():
                    other = plane * across + (column + offset) % across
                    for copy in copies(
                        slot, other, side_send, side_recv, step * across + offset
                    ):
                        copy.start()

            absorb(slot)

        return carry

    lax.fori_loop(0, planes, rise, 0)

    def spread(turn, carry):
        step = turn // (across - 1)
        offset = 1 + turn % (across - 1)

        @pl.when((plane >= step) & ((step > 0) | (column >= offset)))
        def _():
            source = (column + across - offset) % across
            slot = (plane - step) * across + source
            for copy in copies(
                slot, plane * across + source, side_send, side_recv, step * across + offset
            ):
                copy.wait_recv()
            absorb(slot)

        return carry

    lax.fori_loop(0, planes * (across - 1), spread, 0)

    def settle(step, carry):
        @pl.when(plane >= step)
        def _():
            slot = me - step * across

            @pl.when(plane + 1 < planes)
            def _():
                for copy in copies(slot, me + across, up_send, up_recv, step):
                    copy.wait_send()

            for offset in range(1, across):

                @pl.when((step > 0) | (column + offset < across))
                def _():
                    other = plane * across + (column + offset) % across
                    for copy in copies(
                        slot, other, side_send, side_recv, step * across + offset
                    ):
                        copy.wait_send()

        return carry

    lax.fori_loop(0, planes, settle, 0)
    for head in range(heads):
        columns = slice(head * HD, (head + 1) * HD)
        out_ref[:, columns] = (acc[:, columns] / total[head]).astype(out_ref.dtype)


def attend(queries, keys, values, gate_cache, documents):
    tok_rows = queries.shape[0]
    heads = gate_cache.shape[0]
    devices = lax.axis_size("sp")
    planes = min(4, devices)
    across = devices // planes
    aux_rows = (heads + 8) // 8 * 8
    doc_line = documents.astype(jnp.float32)
    packed = jnp.concatenate([keys, values], axis=0)
    aux = jnp.concatenate(
        [
            gate_cache,
            jnp.broadcast_to(doc_line[None, :], (aux_rows - heads, tok_rows)),
        ],
        axis=0,
    )
    vmem = pl.BlockSpec(memory_space=pltpu.VMEM)
    return pl.pallas_call(
        functools.partial(attend_kernel, planes, across),
        out_shape=jax.ShapeDtypeStruct((tok_rows, heads * HD), jnp.bfloat16),
        in_specs=[vmem] * 5,
        out_specs=vmem,
        scratch_shapes=[
            pltpu.VMEM((devices,) + packed.shape, jnp.bfloat16),
            pltpu.VMEM((devices,) + aux.shape, jnp.float32),
            pltpu.VMEM((heads, tok_rows, 1), jnp.float32),
            pltpu.VMEM((heads, tok_rows, 1), jnp.float32),
            pltpu.VMEM((tok_rows, heads * HD), jnp.float32),
            pltpu.SemaphoreType.DMA((2,)),
            pltpu.SemaphoreType.DMA((planes, 2)),
            pltpu.SemaphoreType.DMA((planes, 2)),
            pltpu.SemaphoreType.DMA((planes * across, 2)),
            pltpu.SemaphoreType.DMA((planes * across, 2)),
        ],
        compiler_params=pltpu.CompilerParams(collective_id=0, has_side_effects=True),
        name="attend",
    )(queries, packed, aux, jnp.transpose(gate_cache), doc_line[:, None])


def expert_block(arrived, expert_gate, expert_up, expert_down):
    own_count = expert_gate.shape[0]
    grouped = arrived.reshape(-1, own_count, arrived.shape[1], arrived.shape[2])
    gate_part = jnp.einsum(
        "nemd,edf->nemf", grouped, expert_gate, preferred_element_type=jnp.float32
    )
    up_part = jnp.einsum("nemd,edf->nemf", grouped, expert_up, preferred_element_type=jnp.float32)
    hidden = (jax.nn.silu(gate_part) * up_part).astype(jnp.bfloat16)
    produced = jnp.einsum("nemf,efd->nemd", hidden, expert_down, preferred_element_type=jnp.float32)
    return produced.astype(jnp.bfloat16).reshape(arrived.shape)


def remote(source, target, send_sem, recv_sem, place, core):
    return pltpu.make_async_remote_copy(
        src_ref=source,
        dst_ref=target,
        send_sem=send_sem,
        recv_sem=recv_sem,
        device_id={"sp": place, "tp": core},
        device_id_type=pl.DeviceIdType.MESH,
    )


def greet(barrier, place, core):
    pl.semaphore_signal(
        barrier,
        inc=1,
        device_id={"sp": place, "tp": core},
        device_id_type=pl.DeviceIdType.MESH,
    )


def slot_matrix(meta, first, rows, top_count, weighted):
    width = meta.shape[1]
    row_ids = (first + lax.broadcasted_iota(jnp.int32, (rows, width), 0)).astype(jnp.float32)
    matrix = jnp.zeros((rows, width), jnp.float32)
    for choice in range(top_count):
        filled = meta[top_count + choice : top_count + choice + 1, :] if weighted else 1.0
        matrix = matrix + jnp.where(row_ids == meta[choice : choice + 1, :], filled, 0.0)
    return matrix


def dispatch_kernel(
    planes, across, cores, top_count, chunk, rows_ref, meta_ref, arrived_ref, meta_all,
    blocks, outgoing, own_sem, up_send, up_recv, down_send, down_recv, out_send, out_recv,
):
    group = across * cores
    piece = outgoing.shape[2]
    width = rows_ref.shape[1]
    me, core = lax.axis_index("sp"), lax.axis_index("tp")
    plane, column = me // across, me % across
    seat = column * cores + core

    barrier = pltpu.get_barrier_semaphore()
    for offset in range(1, group):
        other = (seat + offset) % group
        greet(barrier, plane * across + other // cores, other % cores)

    @pl.when(plane + 1 < planes)
    def _():
        greet(barrier, me + across, core)

    @pl.when(plane > 0)
    def _():
        greet(barrier, me - across, core)

    peers = group + 1
    pl.semaphore_wait(barrier, peers - (planes - plane) // planes - (plane + 1) // planes)

    def relay(block, place, send_sem, recv_sem, step):
        return [
            remote(
                ref.at[block], ref.at[block], send_sem.at[step, part], recv_sem.at[step, part],
                place, core,
            )
            for part, ref in enumerate((blocks, meta_all))
        ]

    def pass_up(block, step):
        @pl.when(plane + 1 < planes)
        def _():
            for copy in relay(block, me + across, up_send, up_recv, step):
                copy.start()

    def pass_down(block, step):
        @pl.when(plane > 0)
        def _():
            for copy in relay(block, me - across, down_send, down_recv, step):
                copy.start()

    def piece_copy(block, offset):
        other = (seat + offset) % group
        return remote(
            outgoing.at[block, other],
            arrived_ref.at[block * group + seat],
            out_send.at[block, offset],
            out_recv.at[block, offset],
            plane * across + other // cores,
            other % cores,
        )

    def own_piece(block):
        return pltpu.make_async_copy(
            outgoing.at[block, seat], arrived_ref.at[block * group + seat], out_send.at[block, 0]
        )

    def place_rows(block):
        matrix = slot_matrix(
            meta_all[block], plane * group * piece, group * piece, top_count, False
        ).astype(jnp.bfloat16)
        for start in range(0, width, chunk):
            columns = slice(start, start + chunk)
            placed = jnp.dot(
                matrix, blocks[block, :, columns], preferred_element_type=jnp.float32
            )
            outgoing[block, :, :, columns] = placed.reshape(group, piece, chunk).astype(
                jnp.bfloat16
            )

        def start_piece(offset, carry):
            piece_copy(block, offset).start()
            return carry

        lax.fori_loop(1, group, start_piece, 0)
        own_piece(block).start()

    own = [
        pltpu.make_async_copy(rows_ref, blocks.at[plane], own_sem.at[0]),
        pltpu.make_async_copy(meta_ref, meta_all.at[plane], own_sem.at[1]),
    ]
    for copy in own:
        copy.start()
    for copy in own:
        copy.wait()
    pass_up(plane, 0)
    pass_down(plane, 0)
    place_rows(plane)

    def gather(step, carry):
        @pl.when(plane >= step)
        def _():
            for copy in relay(plane - step, me - across, up_send, up_recv, step - 1):
                copy.wait_recv()
            pass_up(plane - step, step)

        @pl.when(plane + step < planes)
        def _():
            for copy in relay(plane + step, me + across, down_send, down_recv, step - 1):
                copy.wait_recv()
            pass_down(plane + step, step)

        @pl.when(plane >= step)
        def _():
            place_rows(plane - step)

        @pl.when(plane + step < planes)
        def _():
            place_rows(plane + step)

        return carry

    lax.fori_loop(1, planes, gather, 0)

    def settle(step, carry):
        @pl.when((plane >= step) & (plane + 1 < planes))
        def _():
            for copy in relay(plane - step, me + across, up_send, up_recv, step):
                copy.wait_send()

        @pl.when((plane + step < planes) & (plane > 0))
        def _():
            for copy in relay(plane + step, me - across, down_send, down_recv, step):
                copy.wait_send()

        own_piece(step).wait()

        def finish_piece(offset, inner):
            piece_copy(step, offset).wait_send()
            other = (seat + group - offset) % group
            remote(
                outgoing.at[step, other],
                arrived_ref.at[step * group + other],
                out_send.at[step, offset],
                out_recv.at[step, offset],
                plane * across + other // cores,
                other % cores,
            ).wait_recv()
            return inner

        lax.fori_loop(1, group, finish_piece, 0)
        return carry

    lax.fori_loop(0, planes, settle, 0)


def combine_kernel(
    planes, across, cores, top_count, chunk, finished_ref, meta_ref, out_ref,
    back, partial, landed, back_send, back_recv, far_send, far_recv,
):
    group = across * cores
    piece = back.shape[2]
    width = out_ref.shape[1]
    me, core = lax.axis_index("sp"), lax.axis_index("tp")
    plane, column = me // across, me % across
    seat = column * cores + core

    barrier = pltpu.get_barrier_semaphore()
    for offset in range(1, group):
        other = (seat + offset) % group
        greet(barrier, plane * across + other // cores, other % cores)
    for offset in range(1, planes):
        greet(barrier, (plane + offset) % planes * across + column, core)
    pl.semaphore_wait(barrier, group - 1 + planes - 1)

    def piece_copy(block, offset):
        other = (seat + offset) % group
        return remote(
            finished_ref.at[block * group + other],
            back.at[block, seat],
            back_send.at[block, offset],
            back_recv.at[block, offset],
            plane * across + other // cores,
            other % cores,
        )

    def own_piece(block):
        return pltpu.make_async_copy(
            finished_ref.at[block * group + seat], back.at[block, seat], back_send.at[block, 0]
        )

    def far_copy(turn):
        block = (plane + turn) % planes
        return remote(
            partial.at[block], landed.at[turn], far_send.at[turn], far_recv.at[turn],
            block * across + column, core,
        )

    def send_block(turn, carry):
        block = (plane + turn) % planes

        def start_piece(offset, inner):
            piece_copy(block, offset).start()
            return inner

        own_piece(block).start()
        lax.fori_loop(1, group, start_piece, 0)
        return carry

    lax.fori_loop(1, planes + 1, send_block, 0)

    def collect(block, store):
        own_piece(block).wait()

        def wait_piece(offset, inner):
            other = (seat + group - offset) % group
            remote(
                finished_ref.at[block * group + seat],
                back.at[block, other],
                back_send.at[block, offset],
                back_recv.at[block, offset],
                plane * across + other // cores,
                other % cores,
            ).wait_recv()
            return inner

        lax.fori_loop(1, group, wait_piece, 0)
        matrix = jnp.transpose(
            slot_matrix(meta_ref[block], plane * group * piece, group * piece, top_count, True)
        )
        high = matrix.astype(jnp.bfloat16)
        low = (matrix - high.astype(jnp.float32)).astype(jnp.bfloat16)
        for start in range(0, width, chunk):
            columns = slice(start, start + chunk)
            rows = (
                back[block, :, :, columns]
                .astype(jnp.float32)
                .reshape(group * piece, chunk)
                .astype(jnp.bfloat16)
            )
            store(
                columns,
                jnp.dot(high, rows, preferred_element_type=jnp.float32)
                + jnp.dot(low, rows, preferred_element_type=jnp.float32),
            )

    def far_block(turn, carry):
        block = (plane + turn) % planes

        def store(columns, summed):
            partial[block, :, columns] = summed.astype(jnp.bfloat16)

        collect(block, store)
        far_copy(turn).start()
        return carry

    lax.fori_loop(1, planes, far_block, 0)

    def store_own(columns, summed):
        out_ref[:, columns] = summed

    collect(plane, store_own)

    def add_far(turn, carry):
        far_copy(turn).wait_recv()
        for start in range(0, width, chunk):
            columns = slice(start, start + chunk)
            out_ref[:, columns] += landed[turn, :, columns].astype(jnp.float32)
        return carry

    lax.fori_loop(1, planes, add_far, 0)

    def settle(block, carry):
        def finish_piece(offset, inner):
            piece_copy(block, offset).wait_send()
            return inner

        lax.fori_loop(1, group, finish_piece, 0)
        return carry

    lax.fori_loop(0, planes, settle, 0)

    def settle_far(turn, carry):
        far_copy(turn).wait_send()
        return carry

    lax.fori_loop(1, planes, settle_far, 0)


def expert_exchange(settled, slots, route_weight, capacity, expert_weights):
    row_count, width_model = settled.shape
    top_count = route_weight.shape[1]
    places, cores = lax.axis_size("sp"), lax.axis_size("tp")
    planes = min(4, places)
    across = places // planes
    group = across * cores
    piece = capacity * expert_weights[0].shape[0]
    chunk = min(512, width_model)
    meta_rows = (2 * top_count + 7) // 8 * 8
    meta = jnp.concatenate(
        [
            jnp.transpose(slots.reshape(row_count, top_count)).astype(jnp.float32),
            jnp.transpose(route_weight),
            jnp.zeros((meta_rows - 2 * top_count, row_count), jnp.float32),
        ],
        axis=0,
    )
    vmem = pl.BlockSpec(memory_space=pltpu.VMEM)
    anywhere = pl.BlockSpec(memory_space=pl.ANY)
    dma = pltpu.SemaphoreType.DMA
    arrived, meta_all = pl.pallas_call(
        functools.partial(dispatch_kernel, planes, across, cores, top_count, chunk),
        out_shape=(
            jax.ShapeDtypeStruct((places * cores, piece, width_model), jnp.bfloat16),
            jax.ShapeDtypeStruct((planes, meta_rows, row_count), jnp.float32),
        ),
        in_specs=[vmem, vmem],
        out_specs=(anywhere, vmem),
        scratch_shapes=[
            pltpu.VMEM((planes, row_count, width_model), jnp.bfloat16),
            pltpu.VMEM((planes, group, piece, width_model), jnp.bfloat16),
            dma((2,)),
            dma((planes, 2)),
            dma((planes, 2)),
            dma((planes, 2)),
            dma((planes, 2)),
            dma((planes, group)),
            dma((planes, group)),
        ],
        compiler_params=pltpu.CompilerParams(collective_id=1, has_side_effects=True),
        name="dispatch",
    )(settled, meta)
    finished = expert_block(
        arrived.reshape(-1, capacity, width_model), *expert_weights
    ).reshape(arrived.shape)
    return pl.pallas_call(
        functools.partial(combine_kernel, planes, across, cores, top_count, chunk),
        out_shape=jax.ShapeDtypeStruct((row_count, width_model), jnp.float32),
        in_specs=[anywhere, vmem],
        out_specs=vmem,
        scratch_shapes=[
            pltpu.VMEM((planes, group, piece, width_model), jnp.bfloat16),
            pltpu.VMEM((planes, row_count, width_model), jnp.bfloat16),
            pltpu.VMEM((planes, row_count, width_model), jnp.bfloat16),
            dma((planes, group)),
            dma((planes, group)),
            dma((planes,)),
            dma((planes,)),
        ],
        compiler_params=pltpu.CompilerParams(collective_id=2, has_side_effects=True),
        name="combine",
    )(finished, meta_all)


def local(
    queries,
    keys,
    values,
    gate_cache,
    documents,
    residual,
    out_weight,
    mix_gain,
    routes,
    route_weight,
    expert_gate,
    expert_up,
    expert_down,
    shared_gate,
    shared_up,
    shared_down,
    ffn_gain,
):
    attended = attend(queries, keys, values, gate_cache, documents)
    token_heads = lax.all_to_all(attended, "tp", split_axis=0, concat_axis=1, tiled=True)
    mixed = jnp.dot(token_heads, out_weight, preferred_element_type=jnp.float32)
    mixed = lax.optimization_barrier(mixed.astype(jnp.bfloat16)).astype(jnp.float32)
    settled = normalize(residual_scale * residual.astype(jnp.float32) + mixed, mix_gain)
    row_count = settled.shape[0]
    top_count = routes.shape[1]
    expert_total = lax.axis_size(("sp", "tp")) * expert_gate.shape[0]
    capacity = row_count * lax.axis_size("tp") * top_count // expert_total
    chosen_experts = routes.reshape(-1)
    matches = (
        chosen_experts[:, None] == jnp.arange(expert_total, dtype=jnp.int32)[None, :]
    ).astype(jnp.int32)
    ranks = jnp.sum(jnp.cumsum(matches, axis=0) * matches, axis=1) - 1
    slots = chosen_experts * capacity + ranks
    routed = expert_exchange(
        settled, slots, route_weight, capacity, (expert_gate, expert_up, expert_down)
    )
    shared_gate_part = jnp.dot(settled, shared_gate, preferred_element_type=jnp.float32)
    shared_up_part = jnp.dot(settled, shared_up, preferred_element_type=jnp.float32)
    shared_hidden = (jax.nn.silu(shared_gate_part) * shared_up_part).astype(jnp.bfloat16)
    shared = jnp.dot(shared_hidden, shared_down, preferred_element_type=jnp.float32)
    return normalize(residual_scale * settled.astype(jnp.float32) + routed + shared, ffn_gain)


def solution(mesh):
    placed = (
        P("sp", "tp"),
        P("tp", "sp"),
        P("tp", "sp"),
        P("tp", "sp"),
        P("sp"),
        P(("sp", "tp"), None),
        P(),
        P(),
        P(("sp", "tp"), None),
        P(("sp", "tp"), None),
        P(("sp", "tp"), None, None),
        P(("sp", "tp"), None, None),
        P(("sp", "tp"), None, None),
        P(),
        P(),
        P(),
        P(),
    )
    return jax.shard_map(
        local, mesh=mesh, in_specs=placed, out_specs=P(("sp", "tp"), None), check_vma=False
    )
```

```python
import functools

import jax
import jax.numpy as jnp
from jax import lax
from jax.experimental import pallas as pl
from jax.experimental.pallas import tpu as pltpu
from jax.sharding import PartitionSpec as P

HD = 128


residual_scale = 2.0**0.25
norm_epsilon = 1e-05
masked_score = -1e30


def normalize(summed, gain_vector):
    row_mean = jnp.mean(summed, axis=-1, keepdims=True)
    centred = summed - row_mean
    spread = jnp.mean(centred * centred, axis=-1, keepdims=True)
    return (centred * lax.rsqrt(spread + norm_epsilon) * gain_vector.astype(jnp.float32)).astype(
        jnp.bfloat16
    )


def attend_kernel(
    planes, across, q_ref, key_ref, value_ref, aux_ref, gate_ref, doc_ref, out_ref,
    kv_all, aux_all, top, total, acc, own_sem, up_send, up_recv, side_send, side_recv,
):
    heads = gate_ref.shape[1]
    tok_rows = q_ref.shape[0]
    kv_rows = key_ref.shape[0]
    group_size = heads // (kv_rows // HD)
    me = lax.axis_index("sp")
    plane = me // across
    column = me % across

    barrier = pltpu.get_barrier_semaphore()

    def greet(other):
        pl.semaphore_signal(
            barrier, inc=1, device_id={"sp": other}, device_id_type=pl.DeviceIdType.MESH
        )

    for offset in range(1, across):
        greet(plane * across + (column + offset) % across)

    @pl.when(plane + 1 < planes)
    def _():
        greet(me + across)

    @pl.when(plane > 0)
    def _():
        greet(me - across)

    peers = across + 1
    pl.semaphore_wait(
        barrier,
        peers - (planes - plane) // planes - (plane + 1) // planes,
    )

    def copies(slot, other, send_sem, recv_sem, index):
        return [
            pltpu.make_async_remote_copy(
                src_ref=ref.at[slot],
                dst_ref=ref.at[slot],
                send_sem=send_sem.at[index, part],
                recv_sem=recv_sem.at[index, part],
                device_id={"sp": other},
                device_id_type=pl.DeviceIdType.MESH,
            )
            for part, ref in enumerate((kv_all, aux_all))
        ]

    own = [
        pltpu.make_async_copy(key_ref, kv_all.at[me, pl.ds(0, kv_rows)], own_sem.at[0]),
        pltpu.make_async_copy(value_ref, kv_all.at[me, pl.ds(kv_rows, kv_rows)], own_sem.at[2]),
        pltpu.make_async_copy(aux_ref, aux_all.at[me], own_sem.at[1]),
    ]
    for copy in own:
        copy.start()
    top[...] = jnp.full_like(top, masked_score)
    total[...] = jnp.zeros_like(total)
    acc[...] = jnp.zeros_like(acc)
    for copy in own:
        copy.wait()

    def absorb(slot):
        key_pos = slot * tok_rows + lax.broadcasted_iota(jnp.int32, (tok_rows, tok_rows), 1)
        query_pos = me * tok_rows + lax.broadcasted_iota(jnp.int32, (tok_rows, tok_rows), 0)
        allowed = (key_pos <= query_pos) & (aux_all[slot, heads : heads + 1, :] == doc_ref[...])
        for head in range(heads):
            base = head // group_size * HD
            columns = slice(head * HD, (head + 1) * HD)
            key_block = kv_all[slot, base : base + HD, :]
            value_block = kv_all[slot, kv_rows + base : kv_rows + base + HD, :]
            scores = jnp.dot(
                q_ref[:, columns], key_block, preferred_element_type=jnp.float32
            ) * (HD ** (-0.5))
            scores = scores + (gate_ref[:, head : head + 1] - aux_all[slot, head : head + 1, :])
            scores = jnp.where(allowed, scores, masked_score)
            old_top = top[head]
            new_top = jnp.maximum(old_top, jnp.max(scores, axis=1, keepdims=True))
            weights = jnp.exp(scores - new_top)
            shrink = jnp.exp(old_top - new_top)
            top[head] = new_top
            total[head] = total[head] * shrink + jnp.sum(weights, axis=1, keepdims=True)
            acc[:, columns] = acc[:, columns] * shrink + lax.dot_general(
                weights.astype(jnp.bfloat16),
                value_block,
                (((1,), (1,)), ((), ())),
                preferred_element_type=jnp.float32,
            )

    def rise(step, carry):
        @pl.when(plane >= step)
        def _():
            slot = me - step * across

            @pl.when(step > 0)
            def _():
                for copy in copies(slot, me - across, up_send, up_recv, step - 1):
                    copy.wait_recv()

            @pl.when(plane + 1 < planes)
            def _():
                for copy in copies(slot, me + across, up_send, up_recv, step):
                    copy.start()

            for offset in range(1, across):

                @pl.when((step > 0) | (column + offset < across))
                def _():
                    other = plane * across + (column + offset) % across
                    for copy in copies(
                        slot, other, side_send, side_recv, step * across + offset
                    ):
                        copy.start()

            absorb(slot)

        return carry

    lax.fori_loop(0, planes, rise, 0)

    def spread(turn, carry):
        step = turn // (across - 1)
        offset = 1 + turn % (across - 1)

        @pl.when((plane >= step) & ((step > 0) | (column >= offset)))
        def _():
            source = (column + across - offset) % across
            slot = (plane - step) * across + source
            for copy in copies(
                slot, plane * across + source, side_send, side_recv, step * across + offset
            ):
                copy.wait_recv()
            absorb(slot)

        return carry

    lax.fori_loop(0, planes * (across - 1), spread, 0)

    def settle(step, carry):
        @pl.when(plane >= step)
        def _():
            slot = me - step * across

            @pl.when(plane + 1 < planes)
            def _():
                for copy in copies(slot, me + across, up_send, up_recv, step):
                    copy.wait_send()

            for offset in range(1, across):

                @pl.when((step > 0) | (column + offset < across))
                def _():
                    other = plane * across + (column + offset) % across
                    for copy in copies(
                        slot, other, side_send, side_recv, step * across + offset
                    ):
                        copy.wait_send()

        return carry

    lax.fori_loop(0, planes, settle, 0)
    for head in range(heads):
        columns = slice(head * HD, (head + 1) * HD)
        out_ref[:, columns] = (acc[:, columns] / total[head]).astype(out_ref.dtype)


def attend(queries, keys, values, gate_cache, documents):
    tok_rows = queries.shape[0]
    heads = gate_cache.shape[0]
    devices = lax.axis_size("sp")
    planes = min(4, devices)
    across = devices // planes
    aux_rows = (heads + 8) // 8 * 8
    doc_line = documents.astype(jnp.float32)
    aux = jnp.concatenate(
        [
            gate_cache,
            jnp.broadcast_to(doc_line[None, :], (aux_rows - heads, tok_rows)),
        ],
        axis=0,
    )
    vmem = pl.BlockSpec(memory_space=pltpu.VMEM)
    return pl.pallas_call(
        functools.partial(attend_kernel, planes, across),
        out_shape=jax.ShapeDtypeStruct((tok_rows, heads * HD), jnp.bfloat16),
        in_specs=[vmem] * 6,
        out_specs=vmem,
        scratch_shapes=[
            pltpu.VMEM((devices, 2 * keys.shape[0], tok_rows), jnp.bfloat16),
            pltpu.VMEM((devices,) + aux.shape, jnp.float32),
            pltpu.VMEM((heads, tok_rows, 1), jnp.float32),
            pltpu.VMEM((heads, tok_rows, 1), jnp.float32),
            pltpu.VMEM((tok_rows, heads * HD), jnp.float32),
            pltpu.SemaphoreType.DMA((3,)),
            pltpu.SemaphoreType.DMA((planes, 2)),
            pltpu.SemaphoreType.DMA((planes, 2)),
            pltpu.SemaphoreType.DMA((planes * across, 2)),
            pltpu.SemaphoreType.DMA((planes * across, 2)),
        ],
        compiler_params=pltpu.CompilerParams(collective_id=0, has_side_effects=True),
        name="attend",
    )(queries, keys, values, aux, jnp.transpose(gate_cache), doc_line[:, None])


def expert_block(arrived, expert_gate, expert_up, expert_down):
    own_count = expert_gate.shape[0]
    grouped = arrived.reshape(-1, own_count, arrived.shape[1], arrived.shape[2])
    gate_part = jnp.einsum(
        "nemd,edf->nemf", grouped, expert_gate, preferred_element_type=jnp.float32
    )
    up_part = jnp.einsum("nemd,edf->nemf", grouped, expert_up, preferred_element_type=jnp.float32)
    hidden = (jax.nn.silu(gate_part) * up_part).astype(jnp.bfloat16)
    produced = jnp.einsum("nemf,efd->nemd", hidden, expert_down, preferred_element_type=jnp.float32)
    return produced.astype(jnp.bfloat16).reshape(arrived.shape)


def remote(source, target, send_sem, recv_sem, place, core):
    return pltpu.make_async_remote_copy(
        src_ref=source,
        dst_ref=target,
        send_sem=send_sem,
        recv_sem=recv_sem,
        device_id={"sp": place, "tp": core},
        device_id_type=pl.DeviceIdType.MESH,
    )


def greet(barrier, place, core):
    pl.semaphore_signal(
        barrier,
        inc=1,
        device_id={"sp": place, "tp": core},
        device_id_type=pl.DeviceIdType.MESH,
    )


def slot_matrix(meta, first, rows, top_count, weighted):
    width = meta.shape[1]
    row_ids = (first + lax.broadcasted_iota(jnp.int32, (rows, width), 0)).astype(jnp.float32)
    matrix = jnp.zeros((rows, width), jnp.float32)
    for choice in range(top_count):
        filled = meta[top_count + choice : top_count + choice + 1, :] if weighted else 1.0
        matrix = matrix + jnp.where(row_ids == meta[choice : choice + 1, :], filled, 0.0)
    return matrix


def dispatch_kernel(
    planes, across, cores, top_count, chunk, rows_ref, meta_ref, arrived_ref, meta_all,
    blocks, outgoing, own_sem, up_send, up_recv, down_send, down_recv, out_send, out_recv,
):
    group = across * cores
    piece = outgoing.shape[2]
    width = rows_ref.shape[1]
    me, core = lax.axis_index("sp"), lax.axis_index("tp")
    plane, column = me // across, me % across
    seat = column * cores + core

    barrier = pltpu.get_barrier_semaphore()
    for offset in range(1, group):
        other = (seat + offset) % group
        greet(barrier, plane * across + other // cores, other % cores)

    @pl.when(plane + 1 < planes)
    def _():
        greet(barrier, me + across, core)

    @pl.when(plane > 0)
    def _():
        greet(barrier, me - across, core)

    peers = group + 1
    pl.semaphore_wait(barrier, peers - (planes - plane) // planes - (plane + 1) // planes)

    def relay(block, place, send_sem, recv_sem, step):
        return [
            remote(
                ref.at[block], ref.at[block], send_sem.at[step, part], recv_sem.at[step, part],
                place, core,
            )
            for part, ref in enumerate((blocks, meta_all))
        ]

    def pass_up(block, step):
        @pl.when(plane + 1 < planes)
        def _():
            for copy in relay(block, me + across, up_send, up_recv, step):
                copy.start()

    def pass_down(block, step):
        @pl.when(plane > 0)
        def _():
            for copy in relay(block, me - across, down_send, down_recv, step):
                copy.start()

    def piece_copy(block, offset):
        other = (seat + offset) % group
        return remote(
            outgoing.at[block, other],
            arrived_ref.at[block * group + seat],
            out_send.at[block, offset],
            out_recv.at[block, offset],
            plane * across + other // cores,
            other % cores,
        )

    def own_piece(block):
        return pltpu.make_async_copy(
            outgoing.at[block, seat], arrived_ref.at[block * group + seat], out_send.at[block, 0]
        )

    def place_rows(block):
        matrix = slot_matrix(
            meta_all[block], plane * group * piece, group * piece, top_count, False
        ).astype(jnp.bfloat16)
        for start in range(0, width, chunk):
            columns = slice(start, start + chunk)
            placed = jnp.dot(
                matrix, blocks[block, :, columns], preferred_element_type=jnp.float32
            )
            outgoing[block, :, :, columns] = placed.reshape(group, piece, chunk).astype(
                jnp.bfloat16
            )

        def start_piece(offset, carry):
            piece_copy(block, offset).start()
            return carry

        lax.fori_loop(1, group, start_piece, 0)
        own_piece(block).start()

    own = [
        pltpu.make_async_copy(rows_ref, blocks.at[plane], own_sem.at[0]),
        pltpu.make_async_copy(meta_ref, meta_all.at[plane], own_sem.at[1]),
    ]
    for copy in own:
        copy.start()
    for copy in own:
        copy.wait()
    pass_up(plane, 0)
    pass_down(plane, 0)
    place_rows(plane)

    def gather(step, carry):
        @pl.when(plane >= step)
        def _():
            for copy in relay(plane - step, me - across, up_send, up_recv, step - 1):
                copy.wait_recv()
            pass_up(plane - step, step)

        @pl.when(plane + step < planes)
        def _():
            for copy in relay(plane + step, me + across, down_send, down_recv, step - 1):
                copy.wait_recv()
            pass_down(plane + step, step)

        @pl.when(plane >= step)
        def _():
            place_rows(plane - step)

        @pl.when(plane + step < planes)
        def _():
            place_rows(plane + step)

        return carry

    lax.fori_loop(1, planes, gather, 0)

    def settle(step, carry):
        @pl.when((plane >= step) & (plane + 1 < planes))
        def _():
            for copy in relay(plane - step, me + across, up_send, up_recv, step):
                copy.wait_send()

        @pl.when((plane + step < planes) & (plane > 0))
        def _():
            for copy in relay(plane + step, me - across, down_send, down_recv, step):
                copy.wait_send()

        own_piece(step).wait()

        def finish_piece(offset, inner):
            piece_copy(step, offset).wait_send()
            other = (seat + group - offset) % group
            remote(
                outgoing.at[step, other],
                arrived_ref.at[step * group + other],
                out_send.at[step, offset],
                out_recv.at[step, offset],
                plane * across + other // cores,
                other % cores,
            ).wait_recv()
            return inner

        lax.fori_loop(1, group, finish_piece, 0)
        return carry

    lax.fori_loop(0, planes, settle, 0)


def combine_kernel(
    planes, across, cores, top_count, chunk, finished_ref, meta_ref, out_ref,
    back, partial, landed, back_send, back_recv, far_send, far_recv,
):
    group = across * cores
    piece = back.shape[2]
    width = out_ref.shape[1]
    me, core = lax.axis_index("sp"), lax.axis_index("tp")
    plane, column = me // across, me % across
    seat = column * cores + core

    barrier = pltpu.get_barrier_semaphore()
    for offset in range(1, group):
        other = (seat + offset) % group
        greet(barrier, plane * across + other // cores, other % cores)
    for offset in range(1, planes):
        greet(barrier, (plane + offset) % planes * across + column, core)
    pl.semaphore_wait(barrier, group - 1 + planes - 1)

    def piece_copy(block, offset):
        other = (seat + offset) % group
        return remote(
            finished_ref.at[block * group + other],
            back.at[block, seat],
            back_send.at[block, offset],
            back_recv.at[block, offset],
            plane * across + other // cores,
            other % cores,
        )

    def own_piece(block):
        return pltpu.make_async_copy(
            finished_ref.at[block * group + seat], back.at[block, seat], back_send.at[block, 0]
        )

    def far_copy(turn):
        block = (plane + turn) % planes
        return remote(
            partial.at[block], landed.at[turn], far_send.at[turn], far_recv.at[turn],
            block * across + column, core,
        )

    def send_block(turn, carry):
        block = (plane + turn) % planes

        def start_piece(offset, inner):
            piece_copy(block, offset).start()
            return inner

        own_piece(block).start()
        lax.fori_loop(1, group, start_piece, 0)
        return carry

    lax.fori_loop(1, planes + 1, send_block, 0)

    def collect(block, store):
        own_piece(block).wait()

        def wait_piece(offset, inner):
            other = (seat + group - offset) % group
            remote(
                finished_ref.at[block * group + seat],
                back.at[block, other],
                back_send.at[block, offset],
                back_recv.at[block, offset],
                plane * across + other // cores,
                other % cores,
            ).wait_recv()
            return inner

        lax.fori_loop(1, group, wait_piece, 0)
        matrix = jnp.transpose(
            slot_matrix(meta_ref[block], plane * group * piece, group * piece, top_count, True)
        )
        high = matrix.astype(jnp.bfloat16)
        low = (matrix - high.astype(jnp.float32)).astype(jnp.bfloat16)
        for start in range(0, width, chunk):
            columns = slice(start, start + chunk)
            rows = (
                back[block, :, :, columns]
                .astype(jnp.float32)
                .reshape(group * piece, chunk)
                .astype(jnp.bfloat16)
            )
            store(
                columns,
                jnp.dot(high, rows, preferred_element_type=jnp.float32)
                + jnp.dot(low, rows, preferred_element_type=jnp.float32),
            )

    def far_block(turn, carry):
        block = (plane + turn) % planes

        def store(columns, summed):
            partial[block, :, columns] = summed.astype(jnp.bfloat16)

        collect(block, store)
        far_copy(turn).start()
        return carry

    lax.fori_loop(1, planes, far_block, 0)

    def store_own(columns, summed):
        out_ref[:, columns] = summed

    collect(plane, store_own)

    def add_far(turn, carry):
        far_copy(turn).wait_recv()
        for start in range(0, width, chunk):
            columns = slice(start, start + chunk)
            out_ref[:, columns] += landed[turn, :, columns].astype(jnp.float32)
        return carry

    lax.fori_loop(1, planes, add_far, 0)

    def settle(block, carry):
        def finish_piece(offset, inner):
            piece_copy(block, offset).wait_send()
            return inner

        lax.fori_loop(1, group, finish_piece, 0)
        return carry

    lax.fori_loop(0, planes, settle, 0)

    def settle_far(turn, carry):
        far_copy(turn).wait_send()
        return carry

    lax.fori_loop(1, planes, settle_far, 0)


def expert_exchange(settled, slots, route_weight, capacity, expert_weights):
    row_count, width_model = settled.shape
    top_count = route_weight.shape[1]
    places, cores = lax.axis_size("sp"), lax.axis_size("tp")
    planes = min(4, places)
    across = places // planes
    group = across * cores
    piece = capacity * expert_weights[0].shape[0]
    chunk = min(512, width_model)
    meta_rows = (2 * top_count + 7) // 8 * 8
    meta = jnp.concatenate(
        [
            jnp.transpose(slots.reshape(row_count, top_count)).astype(jnp.float32),
            jnp.transpose(route_weight),
            jnp.zeros((meta_rows - 2 * top_count, row_count), jnp.float32),
        ],
        axis=0,
    )
    vmem = pl.BlockSpec(memory_space=pltpu.VMEM)
    anywhere = pl.BlockSpec(memory_space=pl.ANY)
    dma = pltpu.SemaphoreType.DMA
    arrived, meta_all = pl.pallas_call(
        functools.partial(dispatch_kernel, planes, across, cores, top_count, chunk),
        out_shape=(
            jax.ShapeDtypeStruct((places * cores, piece, width_model), jnp.bfloat16),
            jax.ShapeDtypeStruct((planes, meta_rows, row_count), jnp.float32),
        ),
        in_specs=[vmem, vmem],
        out_specs=(anywhere, vmem),
        scratch_shapes=[
            pltpu.VMEM((planes, row_count, width_model), jnp.bfloat16),
            pltpu.VMEM((planes, group, piece, width_model), jnp.bfloat16),
            dma((2,)),
            dma((planes, 2)),
            dma((planes, 2)),
            dma((planes, 2)),
            dma((planes, 2)),
            dma((planes, group)),
            dma((planes, group)),
        ],
        compiler_params=pltpu.CompilerParams(collective_id=1, has_side_effects=True),
        name="dispatch",
    )(settled, meta)
    finished = expert_block(
        arrived.reshape(-1, capacity, width_model), *expert_weights
    ).reshape(arrived.shape)
    return pl.pallas_call(
        functools.partial(combine_kernel, planes, across, cores, top_count, chunk),
        out_shape=jax.ShapeDtypeStruct((row_count, width_model), jnp.float32),
        in_specs=[anywhere, vmem],
        out_specs=vmem,
        scratch_shapes=[
            pltpu.VMEM((planes, group, piece, width_model), jnp.bfloat16),
            pltpu.VMEM((planes, row_count, width_model), jnp.bfloat16),
            pltpu.VMEM((planes, row_count, width_model), jnp.bfloat16),
            dma((planes, group)),
            dma((planes, group)),
            dma((planes,)),
            dma((planes,)),
        ],
        compiler_params=pltpu.CompilerParams(collective_id=2, has_side_effects=True),
        name="combine",
    )(finished, meta_all)


def local(
    queries,
    keys,
    values,
    gate_cache,
    documents,
    residual,
    out_weight,
    mix_gain,
    routes,
    route_weight,
    expert_gate,
    expert_up,
    expert_down,
    shared_gate,
    shared_up,
    shared_down,
    ffn_gain,
):
    attended = attend(queries, keys, values, gate_cache, documents)
    token_heads = lax.all_to_all(attended, "tp", split_axis=0, concat_axis=1, tiled=True)
    mixed = jnp.dot(token_heads, out_weight, preferred_element_type=jnp.float32)
    mixed = lax.optimization_barrier(mixed.astype(jnp.bfloat16)).astype(jnp.float32)
    settled = normalize(residual_scale * residual.astype(jnp.float32) + mixed, mix_gain)
    row_count = settled.shape[0]
    top_count = routes.shape[1]
    expert_total = lax.axis_size(("sp", "tp")) * expert_gate.shape[0]
    capacity = row_count * lax.axis_size("tp") * top_count // expert_total
    chosen_experts = routes.reshape(-1)
    matches = (
        chosen_experts[:, None] == jnp.arange(expert_total, dtype=jnp.int32)[None, :]
    ).astype(jnp.int32)
    ranks = jnp.sum(jnp.cumsum(matches, axis=0) * matches, axis=1) - 1
    slots = chosen_experts * capacity + ranks
    routed = expert_exchange(
        settled, slots, route_weight, capacity, (expert_gate, expert_up, expert_down)
    )
    shared_gate_part = jnp.dot(settled, shared_gate, preferred_element_type=jnp.float32)
    shared_up_part = jnp.dot(settled, shared_up, preferred_element_type=jnp.float32)
    shared_hidden = (jax.nn.silu(shared_gate_part) * shared_up_part).astype(jnp.bfloat16)
    shared = jnp.dot(shared_hidden, shared_down, preferred_element_type=jnp.float32)
    return normalize(residual_scale * settled.astype(jnp.float32) + routed + shared, ffn_gain)


def solution(mesh):
    placed = (
        P("sp", "tp"),
        P("tp", "sp"),
        P("tp", "sp"),
        P("tp", "sp"),
        P("sp"),
        P(("sp", "tp"), None),
        P(),
        P(),
        P(("sp", "tp"), None),
        P(("sp", "tp"), None),
        P(("sp", "tp"), None, None),
        P(("sp", "tp"), None, None),
        P(("sp", "tp"), None, None),
        P(),
        P(),
        P(),
        P(),
    )
    return jax.shard_map(
        local, mesh=mesh, in_specs=placed, out_specs=P(("sp", "tp"), None), check_vma=False
    )
```
